32 devices in a mesh: sp: 8 (over z, x), tp: 4 (over y, core).
Axes of the slice: x: 2, y: 2, z: 4, core: 2. Of those that a mesh axis runs over, the one named last changes fastest.
Arguments:
- stream: bfloat16 [4096, 2048], P('sp', 'tp'), may hold values from -6 to 6
- norm_gain: float32 [2, 2048], replicated, may hold values from 0.1 to 1.9
- w_value: bfloat16 [2, 2048, 2048], P(None, 'sp', 'tp'), may hold values from -0.125 to 0.125
- w_inner: bfloat16 [2, 2048, 2048], P(None, 'sp', 'tp'), may hold values from -0.125 to 0.125
- w_outer: bfloat16 [2, 2048, 2048], P(None, 'sp', 'tp'), may hold values from -0.125 to 0.125
- conv_taps: float32 [2, 3, 2048], P(None, None, 'tp'), may hold values from -3 to 3
- w_output: bfloat16 [2, 2048, 2048], P(None, 'tp', 'sp'), may hold values from -0.125 to 0.125
Outputs:
- result: bfloat16 [4096, 2048], P('sp', 'tp')
The draws below stay inside these ranges and needn't reach their ends.
All inputs are finite; a program needn't handle non-finite values.
Results may differ from the reference program's by a relative error of at most 0.02.
Values may be sent and summed in bfloat16 or wider, within the bound.
A program may use at most 64 MiB of HBM per device.

```python
import jax
import jax.numpy as jnp
from jax import lax

D = 2048
LAYERS = 2
TAPS = 3
TOKENS = 4096
N_TP = 4


def steps_of(stream_key, dims, shards, smallest, largest):
    level, own = 1.0, jax.random.fold_in(stream_key, 6)
    for dim, shards_of in shards:
        heights = jnp.exp(jax.random.uniform(jax.random.fold_in(own, dim), (shards_of,), jnp.float32, smallest / len(shards), largest / len(shards)))
        level = level * jnp.repeat(heights, dims[dim] // shards_of).reshape([-1 if axis == dim else 1 for axis in range(len(dims))])
    return level


def bell_draw(own_key, shape, scale, limit, pieces=(), kind=jnp.bfloat16):
    factor_of = steps_of(own_key, shape, pieces, -0.22, 0.18) if pieces else 1.0
    result = jax.random.normal(own_key, shape, jnp.float32) * scale * factor_of
    return jnp.minimum(jnp.maximum(result, -limit), limit).astype(kind)


def setup_inputs(seed: int = 0) -> dict:
    seeds = jax.random.split(jax.random.key(seed), 8)
    return {
        "stream": bell_draw(seeds[0], (TOKENS, D), 1.0, 6.0, ((0, 8), (1, 4))),
        "norm_gain": jnp.clip(1.0 + 0.18 * jax.random.normal(seeds[1], (LAYERS, D), jnp.float32), 0.1, 1.9),
        "w_value": bell_draw(seeds[2], (LAYERS, D, D), D ** -0.5, 0.125, ((1, 8), (2, 4))),
        "w_inner": bell_draw(seeds[3], (LAYERS, D, D), D ** -0.5, 0.125, ((1, 8), (2, 4))),
        "w_outer": bell_draw(seeds[4], (LAYERS, D, D), D ** -0.5, 0.125, ((1, 8), (2, 4))),
        "conv_taps": bell_draw(seeds[5], (LAYERS, TAPS, D), 0.6, 3.0, ((2, 4),), jnp.float32),
        "w_output": bell_draw(seeds[6], (LAYERS, D, D), D ** -0.5, 0.125, ((1, 4), (2, 8))),
    }


EPSILON = 1e-06

def one_layer(stream_now, gain, weight_value, weight_inner, weight_outer, taps, weight_output):
    stream_float = stream_now.astype(jnp.float32)
    scale = lax.rsqrt(lax.optimization_barrier(jnp.mean(stream_float * stream_float, axis=-1, keepdims=True)) + EPSILON)
    normed = (stream_float * scale * gain).astype(jnp.bfloat16)
    value_proj = jnp.dot(normed, weight_value, preferred_element_type=jnp.float32)
    inner_gate = jnp.dot(normed, weight_inner, preferred_element_type=jnp.float32)
    outer_gate = jnp.dot(normed, weight_outer, preferred_element_type=jnp.float32)
    mixed = (inner_gate * value_proj).astype(jnp.bfloat16)
    row_count = mixed.shape[0]
    padded = jnp.pad(mixed.astype(jnp.float32), ((2, 0), (0, 0)))
    convolved = taps[0] * padded[0:row_count] + taps[1] * padded[1:row_count + 1] + taps[2] * padded[2:]
    gated = (outer_gate * convolved).astype(jnp.bfloat16)
    block_width = gated.shape[1] // N_TP
    summed = jnp.zeros((row_count, gated.shape[1]), jnp.float32)
    for block_index in range(N_TP):
        low = block_index * block_width
        partial_value = jnp.dot(gated[:, low:low + block_width], weight_output[low:low + block_width], preferred_element_type=jnp.float32).astype(jnp.bfloat16)
        partial_value = lax.optimization_barrier(partial_value)
        summed = summed + partial_value.astype(jnp.float32)
    return (stream_float + summed).astype(jnp.bfloat16)

def reference(stream, norm_gain, w_value, w_inner, w_outer, conv_taps, w_output):
    stream_now = stream
    for layer_index in range(LAYERS):
        stream_now = one_layer(stream_now, norm_gain[layer_index], w_value[layer_index], w_inner[layer_index], w_outer[layer_index], conv_taps[layer_index], w_output[layer_index])
    return stream_now
```

```python
import functools

import jax
import jax.numpy as jnp
from jax import lax
from jax.experimental import pallas as pl
from jax.experimental.pallas import tpu as pltpu
from jax.sharding import PartitionSpec as P

EPSILON = 1e-06
MESH = pl.DeviceIdType.MESH
F32 = jnp.float32
BF16 = jnp.bfloat16
HALO = 16


def kernel(
    dims, stream, gain, w_value, w_inner, w_outer, taps, w_output, out,
    win, wout, held, normed, mix, outer, gated, tsend, r1, s1, ra, s2, rb, tail, halo,
    send_sems, own_sems, fwd_sems, relay_sems, w_recv, local_sems, ag_recv, r1_recv,
    ra_recv, rb_recv, halo_recv,
):
    L, SP, TP, D, T, kb, nb, cb = dims
    Z = SP // 2
    half = T // 2
    sp, tp = lax.axis_index("sp"), lax.axis_index("tp")
    z, x = sp // 2, lax.rem(sp, 2)
    q = lax.rem(z, 2)
    y, c = tp // 2, lax.rem(tp, 2)
    x_dev = (sp + 1 - 2 * x, tp)
    y_dev = (sp, tp + 2 - 4 * y)
    c_dev = (sp, tp + 1 - 2 * c)
    pair_dev = (sp + 2 - 4 * q, tp)
    side_dev = (sp - 2 + 4 * q, tp)
    up_dev = (sp + 4, tp)
    down_dev = (sp - 4, tp)
    has_side = jnp.where(q == 0, z, Z - 1 - z) > 0
    has_up, has_down = z + 2 < Z, z >= 2
    tail_out = jnp.logical_and(x == 1, has_up)
    tail_in = jnp.logical_and(x == 0, has_down)
    at_end = jnp.logical_not(has_side)

    sends = []

    def start_if(cond, copy):
        sends.append((cond, copy))
        if cond is None:
            copy().start()
        else:
            @pl.when(cond)
            def _():
                copy().start()

    def remote(src, dst, send_sem, recv_sem, dev):
        return pltpu.make_async_remote_copy(
            src_ref=src, dst_ref=dst, send_sem=send_sem, recv_sem=recv_sem,
            device_id=dev, device_id_type=MESH)

    slots = [0]

    def send(src, dst, recv, dev, cond=None):
        slot = slots[0]
        slots[0] += 1
        start_if(cond, lambda: remote(src, dst, send_sems.at[slot], recv, dev))

    def await_recv(ref, sem):
        remote(ref, ref, send_sems.at[0], sem, x_dev).wait_recv()

    w_in = (w_value, w_inner, w_outer)
    KINDS = 4
    col = lambda p: pl.ds(pl.multiple_of(p * nb, nb), nb)
    krow = lambda s: pl.ds(pl.multiple_of(s * kb, kb), kb)

    def source(l, i, p):
        if i < 3:
            return w_in[i].at[l, :, col(p)]
        return w_output.at[l, col(p), :]

    def part(l, s, i):
        if i < 3:
            return win.at[l, i, krow(s), :]
        return wout.at[l, s]

    def local_copy(l, i):
        return pltpu.make_async_copy(source(l, i, q), part(l, sp, i), local_sems.at[l, i])

    def own_x(l, i):
        start_if(None, lambda: remote(
            source(l, i, q), part(l, sp, i), fwd_sems.at[l, z, i], w_recv.at[l, sp, i], x_dev))

    def own_to(l, i, k, cond, p, dev):
        start_if(cond, lambda: remote(
            source(l, i, p), part(l, sp, i), own_sems.at[l, i, k], w_recv.at[l, sp, i], dev))

    def own_pair(l, i, cond=None):
        own_to(l, i, 0, cond, 1 - q, pair_dev)

    def own_rest(l, i):
        own_to(l, i, 1, has_side, 1 - q, side_dev)
        own_to(l, i, 2, has_up, q, up_dev)
        own_to(l, i, 3, has_down, q, down_dev)

    def take(l, d, i):
        for sign, has_onward, onward in ((-1, has_up, up_dev), (1, has_down, down_dev)):
            origin = z + sign * d
            cond = jnp.logical_and(origin >= 0, origin < Z)
            s = 2 * origin + x

            def forward(s=s, origin=origin):
                ref = part(l, s, i)
                return remote(ref, ref, fwd_sems.at[l, origin, i], w_recv.at[l, s, i], x_dev)

            def relay(s=s, origin=origin, onward=onward):
                ref = part(l, s, i)
                return remote(ref, ref, relay_sems.at[l, origin, i], w_recv.at[l, s, i], onward)

            both = jnp.logical_and(cond, has_onward)
            sends.append((cond, forward))
            sends.append((both, relay))

            @pl.when(cond)
            def _(s=s, forward=forward, relay=relay, has_onward=has_onward):
                await_recv(part(l, s, i), w_recv.at[l, s, i])

                @pl.when(has_onward)
                def _():
                    relay().start()
                forward().start()

    lag = lambda d: (d - 1) // 2
    n_steps = KINDS + lag(Z - 1)

    def take_step(l, k):
        for d in range(1, Z):
            i = k - lag(d)
            if 0 <= i < KINDS:
                take(l, d, i)

    def weights_ready(l, i):
        local_copy(l, i).wait()
        for o in range(Z):
            s = 2 * o + 1 - x
            await_recv(part(l, s, i), w_recv.at[l, s, i])

    rows_of = (pl.ds(0, half), pl.ds(half, half))
    ty, tc, tyc = y_dev[1], c_dev[1], c_dev[1] + 2 - 4 * y

    def spread(l, b, j, h, dev):
        ref = held.at[l, b, j, rows_of[h], :]
        send(ref, ref, ag_recv.at[l, b, j, h], dev)

    def got(l, b, j, h):
        await_recv(held.at[l, b, j, rows_of[h], :], ag_recv.at[l, b, j, h])

    def gather_pair(l, h):
        got(l, 1 - q, tp, h)
        spread(l, 1 - q, tp, h, y_dev)
        spread(l, 1 - q, tp, h, c_dev)

    def gather_y(l, b, h):
        got(l, b, ty, h)
        spread(l, b, ty, h, c_dev)

    def gather_core(l, b):
        for j in (tc, tyc):
            for h in range(2):
                got(l, b, j, h)

    nr = min(128, T)
    per = T // nr

    def normalize(l, b):
        def body(r, carry):
            rows = pl.ds(pl.multiple_of(r * nr, nr), nr)
            blocks = [held[l, b, j, rows, :].astype(F32) for j in range(TP)]
            total = sum(jnp.sum(v * v, axis=-1, keepdims=True) for v in blocks)
            scale = lax.rsqrt(total * (1.0 / D) + EPSILON)
            to = pl.ds(pl.multiple_of(b * T + r * nr, nr), nr)
            for j in range(TP):
                g = gain[l:l + 1, j * cb:(j + 1) * cb]
                normed[to, j * cb:(j + 1) * cb] = (blocks[j] * scale * g).astype(BF16)
            return carry
        lax.fori_loop(0, per, body, 0)

    mb = min(256, T)
    mper = T // mb
    block = lambda b: pl.ds(pl.multiple_of(b * T, T), T)

    def project_mix(l, b):
        n = normed[block(b), :]
        v = jnp.dot(n, win[l, 0], preferred_element_type=F32)
        g = jnp.dot(n, win[l, 1], preferred_element_type=F32)
        m = (g * v).astype(BF16)
        mix[b, HALO:, :] = m.astype(F32)
        tail[l, b] = m[T - HALO:, :]

    def project_outer(l, b):
        n = normed[block(b), :]
        outer[block(b), :] = jnp.dot(n, win[l, 2], preferred_element_type=F32)

    def send_tail(l, b):
        near = jnp.logical_or(x == 0, b == 0)
        far = jnp.logical_and(tail_out, b == 1)
        src, to = tail.at[l, b], jnp.minimum(b + x, 1)
        send(src, halo.at[l, to], halo_recv.at[l, to], x_dev, near)
        send(src, halo.at[l, 0], halo_recv.at[l, 0], (sp + 3, tp), far)

    def convolve(l, b):
        first = jnp.logical_and(jnp.logical_and(x == 0, b == 0), jnp.logical_not(has_down))
        mix[b, 0:HALO, :] = jnp.zeros((HALO, nb), F32)

        @pl.when(jnp.logical_not(first))
        def _():
            await_recv(halo.at[l, b], halo_recv.at[l, b])
            mix[b, 0:HALO, :] = halo[l, b].astype(F32)

        tap = taps[l, :, col(q)]
        o = HALO - 8

        def body(i, carry):
            m = mix[b, pl.ds(pl.multiple_of(o + i * mb, 8), mb + 8), :]
            conv = tap[0:1] * m[6:6 + mb] + tap[1:2] * m[7:7 + mb] + tap[2:3] * m[8:8 + mb]
            rows = pl.ds(pl.multiple_of(b * T + i * mb, mb), mb)
            gated[rows, :] = (outer[rows, :] * conv).astype(BF16)
            return carry
        lax.fori_loop(0, mper, body, 0)

    per_tp = SP // TP

    def w_block(l, j):
        return jnp.concatenate([wout[l, j * per_tp + p] for p in range(per_tp)], axis=1)

    def product(l, b, yj, core):
        return jnp.dot(gated[block(b), :], w_block(l, 2 * yj + core),
                       preferred_element_type=F32).astype(BF16)

    def f(ref):
        return ref.astype(F32)

    order = ((1 - q, 1 - y), (q, 1 - y), (1 - q, y), (q, y))

    def y_first(l, h):
        return l + 1 < L or h == 0

    def outputs(l):
        for b, yj in order:
            tsend[l, b, yj] = product(l, b, yj, 1 - c)
            send(tsend.at[l, b, yj], r1.at[l, b, yj], r1_recv.at[l, b, yj], c_dev)
        for k, (b, yj) in enumerate(order):
            t = product(l, b, yj, c)
            await_recv(r1.at[l, b, yj], r1_recv.at[l, b, yj])
            s1[l, b, yj] = (f(t) + f(r1[l, b, yj])).astype(BF16)
            for h in range(2):
                rows = rows_of[h]
                if y_first(l, h) and k in (0, 1):
                    at, dev = b, y_dev
                elif not y_first(l, h) and k in (0, 2):
                    at, dev = yj, pair_dev
                else:
                    continue
                send(s1.at[l, b, yj, rows, :], ra.at[l, at, rows, :], ra_recv.at[l, at, h], dev)

    def reduce_second(l, h):
        rows = rows_of[h]
        if y_first(l, h):
            at, mine, dev = 1 - q, (1 - q, y), pair_dev
        else:
            at, mine, dev = 1 - y, (q, 1 - y), y_dev
        await_recv(ra.at[l, at, rows, :], ra_recv.at[l, at, h])
        s2[l, rows, :] = (f(s1[l, mine[0], mine[1], rows, :]) + f(ra[l, at, rows, :])).astype(BF16)
        send(s2.at[l, rows, :], rb.at[l, rows, :], rb_recv.at[l, h], dev)

    def reduce_last(l, h):
        rows = rows_of[h]
        at = q if y_first(l, h) else y
        await_recv(ra.at[l, at, rows, :], ra_recv.at[l, at, h])
        await_recv(rb.at[l, rows, :], rb_recv.at[l, h])
        branch = f(s1[l, q, y, rows, :]) + f(ra[l, at, rows, :]) + f(rb[l, rows, :])
        return (f(held[l, q, tp, rows, :]) + branch).astype(BF16)

    def compute(l):
        for b in (q, 1 - q):
            project_mix(l, b)
            send_tail(l, b)
            if b is q:
                weights_ready(l, 2)
            project_outer(l, b)
        turn = jnp.where(x == 1, q, 1 - q)
        convolve(l, turn)
        convolve(l, 1 - turn)

    for l in range(L):
        for i in range(KINDS):
            local_copy(l, i).start()
    held[0, q, tp] = stream[...]

    barrier = pltpu.get_barrier_semaphore()
    count = 4
    for dev in (x_dev, y_dev, c_dev, pair_dev):
        pl.semaphore_signal(barrier, inc=1, device_id=dev, device_id_type=MESH)
    for cond, dev in ((has_side, side_dev), (has_up, up_dev), (has_down, down_dev)):
        count = count + cond.astype(jnp.int32)

        @pl.when(cond)
        def _(dev=dev):
            pl.semaphore_signal(barrier, inc=1, device_id=dev, device_id_type=MESH)

    @pl.when(tail_in)
    def _():
        pl.semaphore_signal(barrier, inc=1, device_id=(sp - 3, tp), device_id_type=MESH)
    pl.semaphore_wait(barrier, count + tail_out.astype(jnp.int32))

    for i in range(KINDS):
        own_x(0, i)
        own_pair(0, i)
        own_rest(0, i)
        if i == 0:
            for h in range(2):
                spread(0, q, tp, h, pair_dev)
                spread(0, q, tp, h, y_dev)
                spread(0, q, tp, h, c_dev)
    for l in range(1, L):
        for i in range(KINDS):
            own_pair(l, i, at_end)

    def gather_rest_start(l):
        for h in range(2):
            gather_pair(l, h)
            gather_y(l, q, h)

    def own_next(l, i):
        own_x(l, i)
        own_rest(l, i)

    not_end = has_side
    for l in range(L):
        more = l + 1 < L
        if l == 0:
            take_step(0, 0)
            take_step(0, 1)
            gather_rest_start(0)
            take_step(0, 2)
            gather_core(0, q)
            normalize(0, q)
            for h in range(2):
                gather_y(0, 1 - q, h)
            for k in range(3, n_steps):
                take_step(0, k)
            gather_core(0, 1 - q)
            normalize(0, 1 - q)
        else:
            gather_core(l, q)
            normalize(l, q)
            for h in range(2):
                gather_y(l, 1 - q, h)
            for k in range(3, n_steps):
                take_step(l, k)
            gather_core(l, 1 - q)
            normalize(l, 1 - q)
        if more:
            for i in range(KINDS):
                own_next(l + 1, i)
            for i in range(2):
                own_pair(l + 1, i, not_end)
        weights_ready(l, 0)
        weights_ready(l, 1)
        compute(l)
        weights_ready(l, 3)
        outputs(l)
        if more:
            take_step(l + 1, 0)
            for h in range(2):
                reduce_second(l, h)
            for i in range(2, KINDS):
                own_pair(l + 1, i, not_end)
            take_step(l + 1, 1)
            for h in range(2):
                held[l + 1, q, tp, rows_of[h], :] = reduce_last(l, h)
                spread(l + 1, q, tp, h, y_dev)
                spread(l + 1, q, tp, h, pair_dev)
                spread(l + 1, q, tp, h, c_dev)
            take_step(l + 1, 2)
            gather_rest_start(l + 1)
        else:
            for h in range(2):
                reduce_second(l, h)
            for h in range(2):
                out[rows_of[h], :] = reduce_last(l, h)

    for cond, copy in sends:
        if cond is None:
            copy().wait_send()
        else:
            @pl.when(cond)
            def _(copy=copy):
                copy().wait_send()


def on_device(SP, TP, stream, norm_gain, w_value, w_inner, w_outer, conv_taps, w_output):
    L, kb, cb = w_value.shape
    T, D = stream.shape[0], norm_gain.shape[1]
    nb, Z = cb // 2, SP // 2
    dims = (L, SP, TP, D, T, kb, nb, cb)
    vmem = pl.BlockSpec(memory_space=pltpu.VMEM)
    hbm = pl.BlockSpec(memory_space=pl.ANY)
    dma = pltpu.SemaphoreType.DMA
    n_sends = L * 28
    return pl.pallas_call(
        functools.partial(kernel, dims),
        out_shape=jax.ShapeDtypeStruct((T, cb), BF16),
        in_specs=[vmem, vmem, hbm, hbm, hbm, vmem, hbm],
        out_specs=vmem,
        scratch_shapes=[
            pltpu.VMEM((L, 3, D, nb), BF16),
            pltpu.VMEM((L, SP, nb, kb), BF16),
            pltpu.VMEM((L, 2, TP, T, cb), BF16),
            pltpu.VMEM((2 * T, D), BF16),
            pltpu.VMEM((2, T + HALO, nb), F32),
            pltpu.VMEM((2 * T, nb), F32),
            pltpu.VMEM((2 * T, nb), BF16),
            pltpu.VMEM((L, 2, 2, T, cb), BF16),
            pltpu.VMEM((L, 2, 2, T, cb), BF16),
            pltpu.VMEM((L, 2, 2, T, cb), BF16),
            pltpu.VMEM((L, 2, T, cb), BF16),
            pltpu.VMEM((L, T, cb), BF16),
            pltpu.VMEM((L, T, cb), BF16),
            pltpu.VMEM((L, 2, HALO, nb), BF16),
            pltpu.VMEM((L, 2, HALO, nb), BF16),
            dma((n_sends,)),
            dma((L, 4, 4)),
            dma((L, Z, 4)),
            dma((L, Z, 4)),
            dma((L, SP, 4)),
            dma((L, 4)),
            dma((L, 2, TP, 2)),
            dma((L, 2, 2)),
            dma((L, 2, 2)),
            dma((L, 2)),
            dma((L, 2)),
        ],
        compiler_params=pltpu.CompilerParams(
            collective_id=0, has_side_effects=True, vmem_limit_bytes=60 * 1024 * 1024
        ),
    )(stream, norm_gain, w_value, w_inner, w_outer, conv_taps, w_output)


def solution(mesh):
    SP, TP = mesh.shape["sp"], mesh.shape["tp"]
    in_specs = (
        P("sp", "tp"),
        P(),
        P(None, "sp", "tp"),
        P(None, "sp", "tp"),
        P(None, "sp", "tp"),
        P(None, None, "tp"),
        P(None, "tp", "sp"),
    )
    return jax.shard_map(
        functools.partial(on_device, SP, TP),
        mesh=mesh, in_specs=in_specs, out_specs=P("sp", "tp"), check_vma=False,
    )
```

```python
import functools

import jax
import jax.numpy as jnp
from jax import lax
from jax.experimental import pallas as pl
from jax.experimental.pallas import tpu as pltpu
from jax.sharding import PartitionSpec as P

EPSILON = 1e-06
MESH = pl.DeviceIdType.MESH
F32 = jnp.float32
BF16 = jnp.bfloat16
HALO = 16


def kernel(
    dims, stream, gain, w_value, w_inner, w_outer, taps, w_output, out,
    win, wout, held, normed, mix, outer, gated, tsend, r1, s1, ra, s2, rb, tail, halo,
    send_sems, own_sems, fwd_sems, relay_sems, w_recv, local_sems, ag_recv, r1_recv,
    ra_recv, rb_recv, halo_recv,
):
    L, SP, TP, D, T, kb, nb, cb = dims
    Z = SP // 2
    half = T // 2
    sp, tp = lax.axis_index("sp"), lax.axis_index("tp")
    z, x = sp // 2, lax.rem(sp, 2)
    q = lax.rem(z, 2)
    y, c = tp // 2, lax.rem(tp, 2)
    x_dev = (sp + 1 - 2 * x, tp)
    y_dev = (sp, tp + 2 - 4 * y)
    c_dev = (sp, tp + 1 - 2 * c)
    pair_dev = (sp + 2 - 4 * q, tp)
    up_dev = (sp + 4, tp)
    down_dev = (sp - 4, tp)
    has_up, has_down = z + 2 < Z, z >= 2
    tail_out = jnp.logical_and(x == 1, has_up)
    tail_in = jnp.logical_and(x == 0, has_down)

    sends = []

    def start_if(cond, copy):
        sends.append((cond, copy))
        if cond is None:
            copy().start()
        else:
            @pl.when(cond)
            def _():
                copy().start()

    def remote(src, dst, send_sem, recv_sem, dev):
        return pltpu.make_async_remote_copy(
            src_ref=src, dst_ref=dst, send_sem=send_sem, recv_sem=recv_sem,
            device_id=dev, device_id_type=MESH)

    slots = [0]

    def send(src, dst, recv, dev, cond=None):
        slot = slots[0]
        slots[0] += 1
        start_if(cond, lambda: remote(src, dst, send_sems.at[slot], recv, dev))

    def await_recv(ref, sem):
        remote(ref, ref, send_sems.at[0], sem, x_dev).wait_recv()

    w_in = (w_value, w_inner, w_outer)
    KINDS = 4
    col = lambda p: pl.ds(pl.multiple_of(p * nb, nb), nb)
    krow = lambda s: pl.ds(pl.multiple_of(s * kb, kb), kb)

    def source(l, i, p):
        if i < 3:
            return w_in[i].at[l, :, col(p)]
        return w_output.at[l, col(p), :]

    def part(l, s, i):
        if i < 3:
            return win.at[l, i, krow(s), :]
        return wout.at[l, s]

    def local_copy(l, i):
        return pltpu.make_async_copy(source(l, i, q), part(l, sp, i), local_sems.at[l, i])

    def own_x(l, i):
        start_if(None, lambda: remote(
            source(l, i, q), part(l, sp, i), fwd_sems.at[l, z, i], w_recv.at[l, sp, i], x_dev))

    def own_to(l, i, k, cond, p, dev):
        start_if(cond, lambda: remote(
            source(l, i, p), part(l, sp, i), own_sems.at[l, i, k], w_recv.at[l, sp, i], dev))

    def inside(o):
        return jnp.logical_and(o >= 0, o < Z)

    reach = lambda l: min(3 if l == 0 else 2, Z - 1)
    ahead = 1 - 2 * q

    def own_z(l, i, way, base):
        for d in range(1, reach(l) + 1):
            step = way * d
            own_to(l, i, base + d - 1, inside(z + step), q if d % 2 == 0 else 1 - q,
                   (sp + 2 * step, tp))

    def toward(l, i):
        own_z(l, i, ahead, 0)

    def away(l, i):
        own_z(l, i, -ahead, 3)

    def take(l, d, i):
        for sign, has_onward, onward in ((-1, has_up, up_dev), (1, has_down, down_dev)):
            origin = z + sign * d
            cond = inside(origin)
            s = 2 * origin + x

            def forward(s=s, origin=origin):
                ref = part(l, s, i)
                return remote(ref, ref, fwd_sems.at[l, origin, i], w_recv.at[l, s, i], x_dev)

            def relay(s=s, origin=origin, onward=onward):
                ref = part(l, s, i)
                return remote(ref, ref, relay_sems.at[l, origin, i], w_recv.at[l, s, i], onward)

            relayed = reach(l) <= d + 1 and d + 2 < Z
            sends.append((cond, forward))
            if relayed:
                sends.append((jnp.logical_and(cond, has_onward), relay))

            @pl.when(cond)
            def _(s=s, forward=forward, relay=relay, has_onward=has_onward):
                await_recv(part(l, s, i), w_recv.at[l, s, i])
                if relayed:
                    @pl.when(has_onward)
                    def _():
                        relay().start()
                forward().start()

    def hop(l, d):
        return 0 if d <= reach(l) else 1 + (d - reach(l) - 1) // 2

    def n_steps(l):
        return KINDS * (1 + hop(l, Z - 1))

    def take_step(l, k):
        for d in range(1, Z):
            if hop(l, d) == k // KINDS:
                take(l, d, k % KINDS)

    def weights_ready(l, i):
        local_copy(l, i).wait()
        for o in range(Z):
            s = 2 * o + 1 - x
            await_recv(part(l, s, i), w_recv.at[l, s, i])

    rows_of = (pl.ds(0, half), pl.ds(half, half))
    ty, tc, tyc = y_dev[1], c_dev[1], c_dev[1] + 2 - 4 * y

    def spread(l, b, j, h, dev):
        ref = held.at[l, b, j, rows_of[h], :]
        send(ref, ref, ag_recv.at[l, b, j, h], dev)

    def got(l, b, j, h):
        await_recv(held.at[l, b, j, rows_of[h], :], ag_recv.at[l, b, j, h])

    def gather_pair(l, h):
        got(l, 1 - q, tp, h)
        spread(l, 1 - q, tp, h, y_dev)
        spread(l, 1 - q, tp, h, c_dev)

    def gather_y(l, b, h):
        got(l, b, ty, h)
        spread(l, b, ty, h, c_dev)

    def gather_core(l, b):
        for j in (tc, tyc):
            for h in range(2):
                got(l, b, j, h)

    nr = min(128, T)
    per = T // nr

    def normalize(l, b):
        def body(r, carry):
            rows = pl.ds(pl.multiple_of(r * nr, nr), nr)
            blocks = [held[l, b, j, rows, :].astype(F32) for j in range(TP)]
            total = sum(jnp.sum(v * v, axis=-1, keepdims=True) for v in blocks)
            scale = lax.rsqrt(total * (1.0 / D) + EPSILON)
            to = pl.ds(pl.multiple_of(b * T + r * nr, nr), nr)
            for j in range(TP):
                g = gain[l:l + 1, j * cb:(j + 1) * cb]
                normed[to, j * cb:(j + 1) * cb] = (blocks[j] * scale * g).astype(BF16)
            return carry
        lax.fori_loop(0, per, body, 0)

    mb = min(256, T)
    mper = T // mb
    block = lambda b: pl.ds(pl.multiple_of(b * T, T), T)

    def project_mix(l, b):
        n = normed[block(b), :]
        v = jnp.dot(n, win[l, 0], preferred_element_type=F32)
        g = jnp.dot(n, win[l, 1], preferred_element_type=F32)
        m = (g * v).astype(BF16)
        mix[b, HALO:, :] = m.astype(F32)
        tail[l, b] = m[T - HALO:, :]

    def project_outer(l, b):
        n = normed[block(b), :]
        outer[block(b), :] = jnp.dot(n, win[l, 2], preferred_element_type=F32)

    def send_tail(l, b):
        near = jnp.logical_or(x == 0, b == 0)
        far = jnp.logical_and(tail_out, b == 1)
        src, to = tail.at[l, b], jnp.minimum(b + x, 1)
        send(src, halo.at[l, to], halo_recv.at[l, to], x_dev, near)
        send(src, halo.at[l, 0], halo_recv.at[l, 0], (sp + 3, tp), far)

    def convolve(l, b):
        first = jnp.logical_and(jnp.logical_and(x == 0, b == 0), jnp.logical_not(has_down))
        mix[b, 0:HALO, :] = jnp.zeros((HALO, nb), F32)

        @pl.when(jnp.logical_not(first))
        def _():
            await_recv(halo.at[l, b], halo_recv.at[l, b])
            mix[b, 0:HALO, :] = halo[l, b].astype(F32)

        tap = taps[l, :, col(q)]
        o = HALO - 8

        def body(i, carry):
            m = mix[b, pl.ds(pl.multiple_of(o + i * mb, 8), mb + 8), :]
            conv = tap[0:1] * m[6:6 + mb] + tap[1:2] * m[7:7 + mb] + tap[2:3] * m[8:8 + mb]
            rows = pl.ds(pl.multiple_of(b * T + i * mb, mb), mb)
            gated[rows, :] = (outer[rows, :] * conv).astype(BF16)
            return carry
        lax.fori_loop(0, mper, body, 0)

    per_tp = SP // TP

    def w_block(l, j):
        return jnp.concatenate([wout[l, j * per_tp + p] for p in range(per_tp)], axis=1)

    def product(l, b, yj, core):
        return jnp.dot(gated[block(b), :], w_block(l, 2 * yj + core),
                       preferred_element_type=F32).astype(BF16)

    def f(ref):
        return ref.astype(F32)

    order = ((1 - q, 1 - y), (q, 1 - y), (1 - q, y), (q, y))

    def y_first(l, h):
        return l + 1 < L or h == 0

    def outputs(l):
        for b, yj in order:
            tsend[l, b, yj] = product(l, b, yj, 1 - c)
            send(tsend.at[l, b, yj], r1.at[l, b, yj], r1_recv.at[l, b, yj], c_dev)
        for k, (b, yj) in enumerate(order):
            t = product(l, b, yj, c)
            await_recv(r1.at[l, b, yj], r1_recv.at[l, b, yj])
            s1[l, b, yj] = (f(t) + f(r1[l, b, yj])).astype(BF16)
            for h in range(2):
                rows = rows_of[h]
                if y_first(l, h) and k in (0, 1):
                    at, dev = b, y_dev
                elif not y_first(l, h) and k in (0, 2):
                    at, dev = yj, pair_dev
                else:
                    continue
                send(s1.at[l, b, yj, rows, :], ra.at[l, at, rows, :], ra_recv.at[l, at, h], dev)

    def reduce_second(l, h):
        rows = rows_of[h]
        if y_first(l, h):
            at, mine, dev = 1 - q, (1 - q, y), pair_dev
        else:
            at, mine, dev = 1 - y, (q, 1 - y), y_dev
        await_recv(ra.at[l, at, rows, :], ra_recv.at[l, at, h])
        s2[l, rows, :] = (f(s1[l, mine[0], mine[1], rows, :]) + f(ra[l, at, rows, :])).astype(BF16)
        send(s2.at[l, rows, :], rb.at[l, rows, :], rb_recv.at[l, h], dev)

    def reduce_last(l, h):
        rows = rows_of[h]
        at = q if y_first(l, h) else y
        await_recv(ra.at[l, at, rows, :], ra_recv.at[l, at, h])
        await_recv(rb.at[l, rows, :], rb_recv.at[l, h])
        branch = f(s1[l, q, y, rows, :]) + f(ra[l, at, rows, :]) + f(rb[l, rows, :])
        return (f(held[l, q, tp, rows, :]) + branch).astype(BF16)

    for l in range(L):
        for i in range(KINDS):
            local_copy(l, i).start()
    held[0, q, tp] = stream[...]

    barrier = pltpu.get_barrier_semaphore()
    count = 4
    for dev in (x_dev, y_dev, c_dev, pair_dev):
        pl.semaphore_signal(barrier, inc=1, device_id=dev, device_id_type=MESH)
    others = [(inside(z - ahead), (sp - 2 * ahead, tp))]
    for d in range(2, reach(0) + 1):
        for way in (-1, 1):
            others.append((inside(z + way * d), (sp + 2 * way * d, tp)))
    for cond, dev in others:
        count = count + cond.astype(jnp.int32)

        @pl.when(cond)
        def _(dev=dev):
            pl.semaphore_signal(barrier, inc=1, device_id=dev, device_id_type=MESH)

    @pl.when(tail_in)
    def _():
        pl.semaphore_signal(barrier, inc=1, device_id=(sp - 3, tp), device_id_type=MESH)
    pl.semaphore_wait(barrier, count + tail_out.astype(jnp.int32))

    def gather_first(l):
        for h in range(2):
            gather_pair(l, h)
            gather_y(l, q, h)

    def gather_last(l):
        for h in range(2):
            gather_y(l, 1 - q, h)

    def project(l, b):
        project_mix(l, b)
        send_tail(l, b)

    def finish(l):
        turn = jnp.where(x == 1, q, 1 - q)
        convolve(l, turn)
        convolve(l, 1 - turn)
        weights_ready(l, 3)
        outputs(l)

    def advance(l, store):
        def step(k):
            if l + 1 < L and k < n_steps(l + 1):
                take_step(l + 1, k)
        step(0)
        step(1)
        reduce_second(l, 0)
        step(2)
        reduce_second(l, 1)
        step(3)
        step(4)
        step(5)
        store(0, reduce_last(l, 0))
        step(6)
        store(1, reduce_last(l, 1))
        step(7)

    for i in range(KINDS):
        own_x(0, i)
        toward(0, i)
        away(0, i)
        if i == 0:
            for h in range(2):
                spread(0, q, tp, h, y_dev)
                spread(0, q, tp, h, c_dev)
        if i < 2:
            spread(0, q, tp, i, pair_dev)
    for l in range(L):
        more = l + 1 < L
        if l == 0:
            take_step(0, 0)
            gather_y(0, q, 0)
            gather_y(0, q, 1)
            gather_pair(0, 0)
            take_step(0, 1)
            gather_pair(0, 1)
            gather_core(0, q)
            normalize(0, q)
            take_step(0, 2)
            gather_last(0)
            gather_core(0, 1 - q)
            normalize(0, 1 - q)
            weights_ready(0, 0)
            weights_ready(0, 1)
            project(0, q)
            project(0, 1 - q)
            if more:
                for i in range(KINDS):
                    toward(1, i)
                    away(1, i)
            for k in range(3, n_steps(l)):
                take_step(0, k)
            if more:
                for i in range(KINDS):
                    own_x(1, i)
            weights_ready(0, 2)
            project_outer(0, q)
            project_outer(0, 1 - q)
        else:
            gather_first(l)
            for k in range(8, n_steps(l)):
                take_step(l, k)
            gather_core(l, q)
            normalize(l, q)
            if more:
                for i in range(KINDS):
                    toward(l + 1, i)
                    away(l + 1, i)
                    own_x(l + 1, i)
            for i in range(3):
                weights_ready(l, i)
            project(l, q)
            project_outer(l, q)
            gather_last(l)
            gather_core(l, 1 - q)
            normalize(l, 1 - q)
            project(l, 1 - q)
            project_outer(l, 1 - q)
        finish(l)
        if more:
            def store(h, value, l=l):
                held[l + 1, q, tp, rows_of[h], :] = value
                spread(l + 1, q, tp, h, y_dev)
                spread(l + 1, q, tp, h, pair_dev)
                spread(l + 1, q, tp, h, c_dev)
            advance(l, store)
        else:
            def store(h, value):
                out[rows_of[h], :] = value
            advance(l, store)

    for cond, copy in sends:
        if cond is None:
            copy().wait_send()
        else:
            @pl.when(cond)
            def _(copy=copy):
                copy().wait_send()


def on_device(SP, TP, stream, norm_gain, w_value, w_inner, w_outer, conv_taps, w_output):
    L, kb, cb = w_value.shape
    T, D = stream.shape[0], norm_gain.shape[1]
    nb, Z = cb // 2, SP // 2
    dims = (L, SP, TP, D, T, kb, nb, cb)
    vmem = pl.BlockSpec(memory_space=pltpu.VMEM)
    hbm = pl.BlockSpec(memory_space=pl.ANY)
    dma = pltpu.SemaphoreType.DMA
    n_sends = L * 28
    return pl.pallas_call(
        functools.partial(kernel, dims),
        out_shape=jax.ShapeDtypeStruct((T, cb), BF16),
        in_specs=[vmem, vmem, hbm, hbm, hbm, vmem, hbm],
        out_specs=vmem,
        scratch_shapes=[
            pltpu.VMEM((L, 3, D, nb), BF16),
            pltpu.VMEM((L, SP, nb, kb), BF16),
            pltpu.VMEM((L, 2, TP, T, cb), BF16),
            pltpu.VMEM((2 * T, D), BF16),
            pltpu.VMEM((2, T + HALO, nb), F32),
            pltpu.VMEM((2 * T, nb), F32),
            pltpu.VMEM((2 * T, nb), BF16),
            pltpu.VMEM((L, 2, 2, T, cb), BF16),
            pltpu.VMEM((L, 2, 2, T, cb), BF16),
            pltpu.VMEM((L, 2, 2, T, cb), BF16),
            pltpu.VMEM((L, 2, T, cb), BF16),
            pltpu.VMEM((L, T, cb), BF16),
            pltpu.VMEM((L, T, cb), BF16),
            pltpu.VMEM((L, 2, HALO, nb), BF16),
            pltpu.VMEM((L, 2, HALO, nb), BF16),
            dma((n_sends,)),
            dma((L, 4, 6)),
            dma((L, Z, 4)),
            dma((L, Z, 4)),
            dma((L, SP, 4)),
            dma((L, 4)),
            dma((L, 2, TP, 2)),
            dma((L, 2, 2)),
            dma((L, 2, 2)),
            dma((L, 2)),
            dma((L, 2)),
        ],
        compiler_params=pltpu.CompilerParams(
            collective_id=0, has_side_effects=True, vmem_limit_bytes=60 * 1024 * 1024
        ),
    )(stream, norm_gain, w_value, w_inner, w_outer, conv_taps, w_output)


def solution(mesh):
    SP, TP = mesh.shape["sp"], mesh.shape["tp"]
    in_specs = (
        P("sp", "tp"),
        P(),
        P(None, "sp", "tp"),
        P(None, "sp", "tp"),
        P(None, "sp", "tp"),
        P(None, None, "tp"),
        P(None, "tp", "sp"),
    )
    return jax.shard_map(
        functools.partial(on_device, SP, TP),
        mesh=mesh, in_specs=in_specs, out_specs=P("sp", "tp"), check_vma=False,
    )
```

```python
import functools

import jax
import jax.numpy as jnp
from jax import lax
from jax.experimental import pallas as pl
from jax.experimental.pallas import tpu as pltpu
from jax.sharding import PartitionSpec as P

EPSILON = 1e-06
MESH = pl.DeviceIdType.MESH
F32 = jnp.float32
BF16 = jnp.bfloat16
HALO = 16
SPLIT = 2


def reach_of(l, k, Z):
    return min(3 if l == 0 or k >= 2 * SPLIT else 2, Z - 1)


def relayed_of(l, k, d, Z):
    return d + 2 < Z and d + 2 > reach_of(l, k, Z)


def relay_slots(L, Z):
    return [(l, d) for l in range(L) for d in range(1, Z)
            if any(relayed_of(l, k, d, Z) for k in range(4 * SPLIT))]


def kernel(
    dims, stream, gain, w_value, w_inner, w_outer, taps, w_output, out,
    win, wout, held, normed, mix, outer, gated, tsend, r1, s1, ra, s2, rb, tail, halo,
    send_sems, own_sems, fwd_sems, relay_sems, z_recv, x_recv, local_sems, ag_recv, core_recv,
    r1_recv, ra_recv, rb_recv, halo_recv,
):
    L, SP, TP, D, T, kb, nb, cb = dims
    Z = SP // 2
    half = T // 2
    sp, tp = lax.axis_index("sp"), lax.axis_index("tp")
    z, x = sp // 2, lax.rem(sp, 2)
    q = lax.rem(z, 2)
    y, c = tp // 2, lax.rem(tp, 2)
    x_dev = (sp + 1 - 2 * x, tp)
    y_dev = (sp, tp + 2 - 4 * y)
    c_dev = (sp, tp + 1 - 2 * c)
    pair_dev = (sp + 2 - 4 * q, tp)
    has_up, has_down = z + 2 < Z, z >= 2
    tail_out = jnp.logical_and(x == 1, has_up)
    tail_in = jnp.logical_and(x == 0, has_down)

    def start_if(cond, copy):
        if cond is None:
            copy().start()
        else:
            @pl.when(cond)
            def _():
                copy().start()

    def remote(src, dst, send_sem, recv_sem, dev):
        return pltpu.make_async_remote_copy(
            src_ref=src, dst_ref=dst, send_sem=send_sem, recv_sem=recv_sem,
            device_id=dev, device_id_type=MESH)

    RELAY, OWN, OWN_CORE, PARTIAL, FIRST, SECOND, TAIL = range(7)

    def send(slot, src, dst, recv, dev, l, cond=None):
        start_if(cond, lambda: remote(src, dst, send_sems.at[l, slot], recv, dev))

    def await_recv(ref, sem):
        remote(ref, ref, send_sems.at[0, 0], sem, x_dev).wait_recv()

    def await_send(ref, sem, cond=None):
        wait = lambda: remote(ref, ref, sem, x_recv.at[0, 0], x_dev).wait_send()
        if cond is None:
            wait()
        else:
            pl.when(cond)(wait)

    w_in = (w_value, w_inner, w_outer)
    KINDS = 4 * SPLIT
    kp, np_ = kb // SPLIT, nb // SPLIT
    col = lambda p: pl.ds(pl.multiple_of(p * nb, nb), nb)

    def source(l, k, p):
        i, r = k // SPLIT, k % SPLIT
        if i < 3:
            return w_in[i].at[l, pl.ds(r * kp, kp), col(p)]
        return w_output.at[l, pl.ds(pl.multiple_of(p * nb + r * np_, np_), np_), :]

    def part(l, s, k):
        i, r = k // SPLIT, k % SPLIT
        if i < 3:
            return win.at[l, i, pl.ds(pl.multiple_of(s * kb + r * kp, kp), kp), :]
        return wout.at[l, s, pl.ds(r * np_, np_), :]

    def local_copy(l, i):
        if i < 3:
            src, dst = w_in[i].at[l, :, col(q)], win.at[l, i, pl.ds(pl.multiple_of(sp * kb, kb), kb), :]
        else:
            src, dst = w_output.at[l, col(q), :], wout.at[l, sp]
        return pltpu.make_async_copy(src, dst, local_sems.at[l, i])

    def own_x(l, k):
        remote(source(l, k, q), part(l, sp, k), fwd_sems.at[l, z], x_recv.at[l, k // SPLIT],
               x_dev).start()

    def own_to(l, i, k, cond, p, dev):
        start_if(cond, lambda: remote(
            source(l, i, p), part(l, sp, i), own_sems.at[l, k], z_recv.at[l, z, i], dev))

    def inside(o):
        return jnp.logical_and(o >= 0, o < Z)

    reach = lambda l, i: reach_of(l, i, Z)
    ahead = 1 - 2 * q

    def own_z(l, i, way, base):
        for d in range(1, reach(l, i) + 1):
            step = way * d
            own_to(l, i, base + d - 1, inside(z + step), q if d % 2 == 0 else 1 - q,
                   (sp + 2 * step, tp))

    def toward(l, i):
        own_z(l, i, ahead, 0)

    def away(l, i):
        own_z(l, i, -ahead, 3)

    relays = relay_slots(L, Z)
    ways = (-ahead, ahead)

    def take(l, i, side, d, who=None):
        way = ways[side]
        origin = z + way * d
        cond = inside(origin)
        if who is not None:
            cond = jnp.logical_and(cond, who)
        s = 2 * origin + x
        ref = part(l, s, i)
        beyond = z - 2 * way
        relayed = relayed_of(l, i, d, Z)
        sem = z_recv.at[l, origin, i]

        @pl.when(cond)
        def _():
            await_recv(ref, sem)
            if relayed:
                @pl.when(inside(beyond))
                def _():
                    remote(ref, ref, relay_sems.at[relays.index((l, d)), side], sem,
                           (2 * beyond + x, tp)).start()
            remote(ref, ref, fwd_sems.at[l, origin], x_recv.at[l, i // SPLIT], x_dev).start()

    def take_pair(l, i, who=None):
        take(l, i, 1, 1, who)

    def take_others(l, i, who=None):
        take(l, i, 0, 1, who)
        for d in range(2, reach(l, i) + 1):
            take(l, i, 1, d, who)
            take(l, i, 0, d, who)

    def take_near(l, *ks):
        for k in ks:
            take_others(l, k)
            take_pair(l, k)

    def take_far(l, *ks):
        for k in ks:
            for d in range(reach(l, k) + 1, Z):
                take(l, k, 1, d)
                take(l, k, 0, d)

    def weights_ready(l, i):
        local_copy(l, i).wait()
        ref = win.at[l, i, pl.ds(0, Z * kb), :] if i < 3 else wout.at[l, pl.ds(0, Z)]
        await_recv(ref, x_recv.at[l, i])

    def pieces(*matrices):
        return [i * SPLIT + r for i in matrices for r in range(SPLIT)]

    def issue(l, *matrices):
        for k in pieces(*matrices):
            toward(l, k)
            away(l, k)

    rows_of = (pl.ds(0, half), pl.ds(half, half))
    ty = y_dev[1]

    FROM_PAIR, FROM_Y = 0, 1

    def spread(slot, l, b, h, to, cond=None):
        ref = held.at[l, b, tp, rows_of[h], :]
        send(slot, ref, ref, ag_recv.at[l, b, to, h], (pair_dev, y_dev)[to], l, cond)

    def to_core(slot, l, b, j, h):
        ref = held.at[l, b, j, rows_of[h], :]
        send(slot, ref, ref, core_recv.at[l, b], c_dev, l)

    def got(l, b, j, h, origin):
        await_recv(held.at[l, b, j, rows_of[h], :], ag_recv.at[l, b, origin, h])

    def spread_own(l, h):
        spread(OWN, l, q, h, FROM_Y)
        to_core(OWN_CORE, l, q, tp, h)

    def gather_pair(l, h):
        got(l, 1 - q, tp, h, FROM_PAIR)
        spread(RELAY, l, 1 - q, h, FROM_Y)
        to_core(RELAY, l, 1 - q, tp, h)

    def gather_y(l, b, h):
        got(l, b, ty, h, FROM_Y)
        to_core(RELAY, l, b, ty, h)

    def gather_core(l, b):
        await_recv(held.at[l, b, pl.ds(0, 2)], core_recv.at[l, b])

    nr = min(128, T)
    per = T // nr

    def normalize(l, b):
        def body(r, carry):
            rows = pl.ds(pl.multiple_of(r * nr, nr), nr)
            blocks = [held[l, b, j, rows, :].astype(F32) for j in range(TP)]
            total = sum(jnp.sum(v * v, axis=-1, keepdims=True) for v in blocks)
            scale = lax.rsqrt(total * (1.0 / D) + EPSILON)
            to = pl.ds(pl.multiple_of(b * T + r * nr, nr), nr)
            for j in range(TP):
                g = gain[l:l + 1, j * cb:(j + 1) * cb]
                normed[to, j * cb:(j + 1) * cb] = (blocks[j] * scale * g).astype(BF16)
            return carry
        lax.fori_loop(0, per, body, 0)

    mb = min(256, T)
    mper = T // mb
    block = lambda b: pl.ds(pl.multiple_of(b * T, T), T)

    def project_mix(l, b):
        n = normed[block(b), :]
        v = jnp.dot(n, win[l, 0], preferred_element_type=F32)
        g = jnp.dot(n, win[l, 1], preferred_element_type=F32)
        m = (g * v).astype(BF16)
        mix[b, HALO:, :] = m.astype(F32)
        tail[l, b] = m[T - HALO:, :]

    def project_outer(l, b):
        n = normed[block(b), :]
        outer[block(b), :] = jnp.dot(n, win[l, 2], preferred_element_type=F32)

    def send_tail(l, b, n):
        near = jnp.logical_or(x == 0, b == 0)
        far = jnp.logical_and(tail_out, b == 1)
        src, to = tail.at[l, b], jnp.minimum(b + x, 1)
        send(TAIL + n, src, halo.at[l, to], halo_recv.at[l, to], x_dev, l, near)
        send(TAIL + n, src, halo.at[l, 0], halo_recv.at[l, 0], (sp + 3, tp), l, far)

    def convolve(l, b):
        first = jnp.logical_and(jnp.logical_and(x == 0, b == 0), jnp.logical_not(has_down))
        mix[b, 0:HALO, :] = jnp.zeros((HALO, nb), F32)

        @pl.when(jnp.logical_not(first))
        def _():
            await_recv(halo.at[l, b], halo_recv.at[l, b])
            mix[b, 0:HALO, :] = halo[l, b].astype(F32)

        tap = taps[:, l, col(q)]
        o = HALO - 8

        def body(i, carry):
            m = mix[b, pl.ds(pl.multiple_of(o + i * mb, 8), mb + 8), :]
            conv = tap[0:1] * m[6:6 + mb] + tap[1:2] * m[7:7 + mb] + tap[2:3] * m[8:8 + mb]
            rows = pl.ds(pl.multiple_of(b * T + i * mb, mb), mb)
            gated[rows, :] = (outer[rows, :] * conv).astype(BF16)
            return carry
        lax.fori_loop(0, mper, body, 0)

    per_tp = SP // TP

    def w_block(l, j):
        return jnp.concatenate([wout[l, j * per_tp + p] for p in range(per_tp)], axis=1)

    def product(l, b, yj, core):
        return jnp.dot(gated[block(b), :], w_block(l, 2 * yj + core),
                       preferred_element_type=F32).astype(BF16)

    def f(ref):
        return ref.astype(F32)

    order = ((1 - q, 1 - y), (q, 1 - y), (1 - q, y), (q, y))

    def y_first(l, h):
        return l + 1 < L or h == 0

    def outputs(l):
        for b, yj in order:
            tsend[l, b, yj] = product(l, b, yj, 1 - c)
            send(PARTIAL, tsend.at[l, b, yj], r1.at[l, b, yj], r1_recv.at[l, b, yj], c_dev, l)
        for k, (b, yj) in enumerate(order):
            t = product(l, b, yj, c)
            await_recv(r1.at[l, b, yj], r1_recv.at[l, b, yj])
            s1[l, b, yj] = (f(t) + f(r1[l, b, yj])).astype(BF16)
            for h in range(2):
                rows = rows_of[h]
                if y_first(l, h) and k in (0, 1):
                    at, dev = b, y_dev
                elif not y_first(l, h) and k in (0, 2):
                    at, dev = yj, pair_dev
                else:
                    continue
                send(FIRST, s1.at[l, b, yj, rows, :], ra.at[l, at, rows, :],
                     ra_recv.at[l, at, h], dev, l)

    def reduce_second(l, h):
        rows = rows_of[h]
        if y_first(l, h):
            at, mine, dev = 1 - q, (1 - q, y), pair_dev
        else:
            at, mine, dev = 1 - y, (q, 1 - y), y_dev
        await_recv(ra.at[l, at, rows, :], ra_recv.at[l, at, h])
        s2[l, rows, :] = (f(s1[l, mine[0], mine[1], rows, :]) + f(ra[l, at, rows, :])).astype(BF16)
        send(SECOND, s2.at[l, rows, :], rb.at[l, rows, :], rb_recv.at[l, h], dev, l)

    def reduce_last(l, h):
        rows = rows_of[h]
        at = q if y_first(l, h) else y
        await_recv(ra.at[l, at, rows, :], ra_recv.at[l, at, h])
        await_recv(rb.at[l, rows, :], rb_recv.at[l, h])
        branch = f(s1[l, q, y, rows, :]) + f(ra[l, at, rows, :]) + f(rb[l, rows, :])
        return (f(held[l, q, tp, rows, :]) + branch).astype(BF16)

    for l in range(L):
        for i in range(4):
            local_copy(l, i).start()
    held[0, q, tp] = stream[...]

    barrier = pltpu.get_barrier_semaphore()
    count = 4
    for dev in (x_dev, y_dev, c_dev, pair_dev):
        pl.semaphore_signal(barrier, inc=1, device_id=dev, device_id_type=MESH)
    others = [(inside(z - ahead), (sp - 2 * ahead, tp))]
    for d in range(2, reach(0, 0) + 1):
        for way in (-1, 1):
            others.append((inside(z + way * d), (sp + 2 * way * d, tp)))
    for cond, dev in others:
        count = count + cond.astype(jnp.int32)

        @pl.when(cond)
        def _(dev=dev):
            pl.semaphore_signal(barrier, inc=1, device_id=dev, device_id_type=MESH)

    @pl.when(tail_in)
    def _():
        pl.semaphore_signal(barrier, inc=1, device_id=(sp - 3, tp), device_id_type=MESH)
    pl.semaphore_wait(barrier, count + tail_out.astype(jnp.int32))

    def gather_first(l):
        for h in range(2):
            gather_pair(l, h)
            gather_y(l, q, h)

    def gather_last(l):
        for h in range(2):
            gather_y(l, 1 - q, h)

    def project(l, b):
        project_mix(l, b)
        send_tail(l, b, 0 if b is q else 1)

    def finish(l):
        turn = jnp.where(x == 1, q, 1 - q)
        convolve(l, turn)
        convolve(l, 1 - turn)
        weights_ready(l, 3)
        outputs(l)

    def flush_weights(l):
        size = lambda n: win.at[l, 0, pl.ds(0, n * kp), :]
        for side in range(2):
            for d in range(1, Z):
                to = z + ways[side] * d
                n = sum(d <= reach(l, k) for k in range(KINDS))
                if n:
                    await_send(size(n), own_sems.at[l, 3 * (1 - side) + d - 1], inside(to))
                n = sum(relayed_of(l, k, d, Z) for k in range(KINDS))
                if n:
                    both = jnp.logical_and(inside(to), inside(z - 2 * ways[side]))
                    await_send(size(n), relay_sems.at[relays.index((l, d)), side], both)
        for o in range(Z):
            await_send(size(KINDS), fwd_sems.at[l, o])

    def flush_gather(l):
        await_send(held.at[l, 0], send_sems.at[l, RELAY])
        await_send(ra.at[l], send_sems.at[l, OWN])
        await_send(rb.at[l], send_sems.at[l, OWN_CORE])

    def flush_layer(l):
        await_send(tsend.at[l], send_sems.at[l, PARTIAL])
        await_send(ra.at[l], send_sems.at[l, FIRST])
        await_send(rb.at[l], send_sems.at[l, SECOND])
        for n, b in ((0, q), (1, 1 - q)):
            near = jnp.logical_or(x == 0, b == 0)
            far = jnp.logical_and(tail_out, b == 1)
            await_send(tail.at[l, 0], send_sems.at[l, TAIL + n], jnp.logical_or(near, far))

    def advance(l, store):
        n = l + 1
        if n == L:
            for h in range(2):
                reduce_second(l, h)
            for m in range(L):
                flush_weights(m)
                flush_gather(m)
                if m < l:
                    flush_layer(m)
            for h in range(2):
                store(h, reduce_last(l, h))
            return
        issue(n, 2)
        take_near(n, *pieces(0, 1))
        for h in range(2):
            reduce_second(l, h)
        take_far(n, *pieces(0))
        store(0, reduce_last(l, 0))
        take_far(n, *pieces(1))
        store(1, reduce_last(l, 1))
        take_near(n, *pieces(2))
        take_far(n, *pieces(2))

    inner = inside(z - ahead)
    outer_end = jnp.logical_not(inner)
    for h in range(2):
        spread_own(0, h)
    for k in range(KINDS):
        own_x(0, k)
        toward(0, k)
        away(0, k)
        if k == SPLIT - 1:
            spread(OWN, 0, q, 0, FROM_PAIR)
            spread(OWN, 0, q, 1, FROM_PAIR, inner)
        if k == 2 * SPLIT - 1:
            spread(OWN, 0, q, 1, FROM_PAIR, outer_end)

    def first_arrivals():
        for k in range(SPLIT):
            take_near(0, k)
        for h in range(2):
            gather_y(0, q, h)
        for k in range(SPLIT, 2 * SPLIT):
            take_others(0, k)
            take_pair(0, k, inner)
            if k == SPLIT:
                gather_pair(0, 0)
                gather_core(0, q)
                normalize(0, q)
        for k in pieces(2)[:1]:
            take_others(0, k, inner)
            take_pair(0, k, inner)
        gather_pair(0, 1)
        for k in pieces(2)[:1]:
            take_others(0, k, outer_end)
        for k in pieces(1) + pieces(2)[:1]:
            take_pair(0, k, outer_end)
        take_near(0, *pieces(2)[1:])
        gather_last(0)
        take_near(0, *pieces(3)[:-1])
        gather_core(0, 1 - q)
        normalize(0, 1 - q)
        weights_ready(0, 0)
        weights_ready(0, 1)
        project(0, q)
        take_near(0, *pieces(3)[-1:])
        take_far(0, *range(KINDS))
        project(0, 1 - q)

    for l in range(L):
        more = l + 1 < L
        if l == 0:
            first_arrivals()
            if more:
                issue(1, 0, 1)
                for k in range(KINDS):
                    own_x(1, k)
            weights_ready(0, 2)
            project_outer(0, q)
            project_outer(0, 1 - q)
        else:
            for h in range(2):
                gather_pair(l, h)
                gather_y(l, q, h)
                if h == 0:
                    issue(l, 3)
            gather_core(l, q)
            normalize(l, q)
            if more:
                issue(l + 1, 0, 1)
                for k in range(KINDS):
                    own_x(l + 1, k)
            for i in range(3):
                weights_ready(l, i)
            project(l, q)
            project_outer(l, q)
            take_near(l, *pieces(3))
            take_far(l, *pieces(3))
            gather_last(l)
            gather_core(l, 1 - q)
            normalize(l, 1 - q)
            project(l, 1 - q)
            project_outer(l, 1 - q)
        finish(l)
        if more:
            def store(h, value, l=l):
                held[l + 1, q, tp, rows_of[h], :] = value
                spread(OWN, l + 1, q, h, FROM_PAIR)
                spread_own(l + 1, h)
            advance(l, store)
        else:
            def store(h, value):
                out[rows_of[h], :] = value
            advance(l, store)

    flush_layer(L - 1)


def on_device(SP, TP, stream, norm_gain, w_value, w_inner, w_outer, conv_taps, w_output):
    L, kb, cb = w_value.shape
    T, D = stream.shape[0], norm_gain.shape[1]
    nb, Z = cb // 2, SP // 2
    dims = (L, SP, TP, D, T, kb, nb, cb)
    vmem = pl.BlockSpec(memory_space=pltpu.VMEM)
    hbm = pl.BlockSpec(memory_space=pl.ANY)
    dma = pltpu.SemaphoreType.DMA
    kinds = 4 * SPLIT
    n_relays = max(1, len(relay_slots(L, Z)))
    return pl.pallas_call(
        functools.partial(kernel, dims),
        out_shape=jax.ShapeDtypeStruct((T, cb), BF16),
        in_specs=[vmem, vmem, hbm, hbm, hbm, vmem, hbm],
        out_specs=vmem,
        scratch_shapes=[
            pltpu.VMEM((L, 3, D, nb), BF16),
            pltpu.VMEM((L, SP, nb, kb), BF16),
            pltpu.VMEM((L, 2, TP, T, cb), BF16),
            pltpu.VMEM((2 * T, D), BF16),
            pltpu.VMEM((2, T + HALO, nb), F32),
            pltpu.VMEM((2 * T, nb), F32),
            pltpu.VMEM((2 * T, nb), BF16),
            pltpu.VMEM((L, 2, 2, T, cb), BF16),
            pltpu.VMEM((L, 2, 2, T, cb), BF16),
            pltpu.VMEM((L, 2, 2, T, cb), BF16),
            pltpu.VMEM((L, 2, T, cb), BF16),
            pltpu.VMEM((L, T, cb), BF16),
            pltpu.VMEM((L, T, cb), BF16),
            pltpu.VMEM((L, 2, HALO, nb), BF16),
            pltpu.VMEM((L, 2, HALO, nb), BF16),
            dma((L, 8)),
            dma((L, 6)),
            dma((L, Z)),
            dma((n_relays, 2)),
            dma((L, Z, kinds)),
            dma((L, 4)),
            dma((L, 4)),
            dma((L, 2, 2, 2)),
            dma((L, 2)),
            dma((L, 2, 2)),
            dma((L, 2, 2)),
            dma((L, 2)),
            dma((L, 2)),
        ],
        compiler_params=pltpu.CompilerParams(
            collective_id=0, has_side_effects=True, vmem_limit_bytes=60 * 1024 * 1024
        ),
    )(stream, norm_gain, w_value, w_inner, w_outer, jnp.transpose(conv_taps, (1, 0, 2)), w_output)


def solution(mesh):
    SP, TP = mesh.shape["sp"], mesh.shape["tp"]
    in_specs = (
        P("sp", "tp"),
        P(),
        P(None, "sp", "tp"),
        P(None, "sp", "tp"),
        P(None, "sp", "tp"),
        P(None, None, "tp"),
        P(None, "tp", "sp"),
    )
    return jax.shard_map(
        functools.partial(on_device, SP, TP),
        mesh=mesh, in_specs=in_specs, out_specs=P("sp", "tp"), check_vma=False,
    )
```

```python
import functools

import jax
import jax.numpy as jnp
from jax import lax
from jax.experimental import pallas as pl
from jax.experimental.pallas import tpu as pltpu
from jax.sharding import PartitionSpec as P

EPSILON = 1e-06
MESH = pl.DeviceIdType.MESH
F32 = jnp.float32
BF16 = jnp.bfloat16
HALO = 16
SPLIT = 2


def reach_of(l, k, Z):
    return min(3 if l == 0 or k >= 2 * SPLIT else 2, Z - 1)


def relayed_of(l, k, d, Z):
    return d + 2 < Z and d + 2 > reach_of(l, k, Z)


def relay_slots(L, Z):
    return [(l, d) for l in range(L) for d in range(1, Z)
            if any(relayed_of(l, k, d, Z) for k in range(4 * SPLIT))]


def kernel(
    dims, stream, gain, w_value, w_inner, w_outer, taps, w_output, out,
    win, wout, held, normed, mix, outer, gated, tsend, r1, s1, ra, s2, rb, tail, halo,
    send_sems, own_sems, fwd_sems, relay_sems, z_recv, x_recv, local_sems, ag_recv, core_recv,
    r1_recv, ra_recv, rb_recv, halo_recv,
):
    L, SP, TP, D, T, kb, nb, cb = dims
    Z = SP // 2
    half = T // 2
    sp, tp = lax.axis_index("sp"), lax.axis_index("tp")
    z, x = sp // 2, lax.rem(sp, 2)
    q = lax.rem(z, 2)
    y, c = tp // 2, lax.rem(tp, 2)
    x_dev = (sp + 1 - 2 * x, tp)
    y_dev = (sp, tp + 2 - 4 * y)
    c_dev = (sp, tp + 1 - 2 * c)
    pair_dev = (sp + 2 - 4 * q, tp)
    has_up, has_down = z + 2 < Z, z >= 2
    tail_out = jnp.logical_and(x == 1, has_up)
    tail_in = jnp.logical_and(x == 0, has_down)

    def start_if(cond, copy):
        if cond is None:
            copy().start()
        else:
            @pl.when(cond)
            def _():
                copy().start()

    def remote(src, dst, send_sem, recv_sem, dev):
        return pltpu.make_async_remote_copy(
            src_ref=src, dst_ref=dst, send_sem=send_sem, recv_sem=recv_sem,
            device_id=dev, device_id_type=MESH)

    RELAY, OWN, OWN_CORE, PARTIAL, FIRST, SECOND, TAIL = range(7)

    def send(slot, src, dst, recv, dev, l, cond=None):
        start_if(cond, lambda: remote(src, dst, send_sems.at[l, slot], recv, dev))

    def await_recv(ref, sem):
        remote(ref, ref, send_sems.at[0, 0], sem, x_dev).wait_recv()

    def await_send(ref, sem, cond=None):
        wait = lambda: remote(ref, ref, sem, x_recv.at[0, 0], x_dev).wait_send()
        if cond is None:
            wait()
        else:
            pl.when(cond)(wait)

    w_in = (w_value, w_inner, w_outer)
    KINDS = 4 * SPLIT
    kp, np_ = kb // SPLIT, nb // SPLIT
    col = lambda p: pl.ds(pl.multiple_of(p * nb, nb), nb)

    def source(l, k, p):
        i, r = k // SPLIT, k % SPLIT
        if i < 3:
            return w_in[i].at[l, pl.ds(r * kp, kp), col(p)]
        return w_output.at[l, pl.ds(pl.multiple_of(p * nb + r * np_, np_), np_), :]

    def part(l, s, k):
        i, r = k // SPLIT, k % SPLIT
        if i < 3:
            return win.at[l, i, pl.ds(pl.multiple_of(s * kb + r * kp, kp), kp), :]
        return wout.at[l, s, pl.ds(r * np_, np_), :]

    def local_copy(l, i):
        if i < 3:
            src, dst = w_in[i].at[l, :, col(q)], win.at[l, i, pl.ds(pl.multiple_of(sp * kb, kb), kb), :]
        else:
            src, dst = w_output.at[l, col(q), :], wout.at[l, sp]
        return pltpu.make_async_copy(src, dst, local_sems.at[l, i])

    def own_x(l, k):
        remote(source(l, k, q), part(l, sp, k), fwd_sems.at[l, z], x_recv.at[l, k // SPLIT],
               x_dev).start()

    def own_to(l, i, k, cond, p, dev):
        start_if(cond, lambda: remote(
            source(l, i, p), part(l, sp, i), own_sems.at[l, k], z_recv.at[l, z, i], dev))

    def inside(o):
        return jnp.logical_and(o >= 0, o < Z)

    reach = lambda l, i: reach_of(l, i, Z)
    ahead = 1 - 2 * q

    def own_z(l, i, way, base):
        for d in range(1, reach(l, i) + 1):
            step = way * d
            own_to(l, i, base + d - 1, inside(z + step), q if d % 2 == 0 else 1 - q,
                   (sp + 2 * step, tp))

    def toward(l, i):
        own_z(l, i, ahead, 0)

    def away(l, i):
        own_z(l, i, -ahead, 3)

    relays = relay_slots(L, Z)
    ways = (-ahead, ahead)

    def take(l, i, side, d, who=None):
        way = ways[side]
        origin = z + way * d
        cond = inside(origin)
        if who is not None:
            cond = jnp.logical_and(cond, who)
        s = 2 * origin + x
        ref = part(l, s, i)
        beyond = z - 2 * way
        relayed = relayed_of(l, i, d, Z)
        sem = z_recv.at[l, origin, i]

        @pl.when(cond)
        def _():
            await_recv(ref, sem)
            if relayed:
                @pl.when(inside(beyond))
                def _():
                    remote(ref, ref, relay_sems.at[relays.index((l, d)), side], sem,
                           (2 * beyond + x, tp)).start()
            remote(ref, ref, fwd_sems.at[l, origin], x_recv.at[l, i // SPLIT], x_dev).start()

    def take_pair(l, i, who=None):
        take(l, i, 1, 1, who)

    def take_others(l, i, who=None):
        take(l, i, 0, 1, who)
        for d in range(2, reach(l, i) + 1):
            take(l, i, 1, d, who)
            take(l, i, 0, d, who)

    def take_near(l, *ks):
        for k in ks:
            take_others(l, k)
            take_pair(l, k)

    def take_far(l, *ks):
        for k in ks:
            for d in range(reach(l, k) + 1, Z):
                take(l, k, 1, d)
                take(l, k, 0, d)

    def weights_ready(l, i):
        local_copy(l, i).wait()
        ref = win.at[l, i, pl.ds(0, Z * kb), :] if i < 3 else wout.at[l, pl.ds(0, Z)]
        await_recv(ref, x_recv.at[l, i])

    def pieces(*matrices):
        return [i * SPLIT + r for i in matrices for r in range(SPLIT)]

    def issue(l, *matrices):
        for k in pieces(*matrices):
            toward(l, k)
            away(l, k)

    rows_of = (pl.ds(0, half), pl.ds(half, half))
    ty = y_dev[1]

    FROM_PAIR, FROM_Y = 0, 1

    def spread(slot, l, b, h, to, cond=None):
        ref = held.at[l, b, tp, rows_of[h], :]
        send(slot, ref, ref, ag_recv.at[l, b, to, h], (pair_dev, y_dev)[to], l, cond)

    def to_core(slot, l, b, j, h):
        ref = held.at[l, b, j, rows_of[h], :]
        send(slot, ref, ref, core_recv.at[l, b], c_dev, l)

    def got(l, b, j, h, origin):
        await_recv(held.at[l, b, j, rows_of[h], :], ag_recv.at[l, b, origin, h])

    def spread_own(l, h):
        spread(OWN, l, q, h, FROM_Y)
        to_core(OWN_CORE, l, q, tp, h)

    def gather_pair(l, h):
        got(l, 1 - q, tp, h, FROM_PAIR)
        spread(RELAY, l, 1 - q, h, FROM_Y)
        to_core(RELAY, l, 1 - q, tp, h)

    def gather_y(l, b, h):
        got(l, b, ty, h, FROM_Y)
        to_core(RELAY, l, b, ty, h)

    def gather_core(l, b):
        await_recv(held.at[l, b, pl.ds(0, 2)], core_recv.at[l, b])

    nr = min(128, T)
    per = T // nr

    def normalize(l, b):
        def body(r, carry):
            rows = pl.ds(pl.multiple_of(r * nr, nr), nr)
            blocks = [held[l, b, j, rows, :].astype(F32) for j in range(TP)]
            total = sum(jnp.sum(v * v, axis=-1, keepdims=True) for v in blocks)
            scale = lax.rsqrt(total * (1.0 / D) + EPSILON)
            to = pl.ds(pl.multiple_of(b * T + r * nr, nr), nr)
            for j in range(TP):
                g = gain[l:l + 1, j * cb:(j + 1) * cb]
                normed[to, j * cb:(j + 1) * cb] = (blocks[j] * scale * g).astype(BF16)
            return carry
        lax.fori_loop(0, per, body, 0)

    mb = min(256, T)
    mper = T // mb
    block = lambda b: pl.ds(pl.multiple_of(b * T, T), T)

    def project_mix(l, b):
        n = normed[block(b), :]
        v = jnp.dot(n, win[l, 0], preferred_element_type=F32)
        g = jnp.dot(n, win[l, 1], preferred_element_type=F32)
        m = (g * v).astype(BF16)
        mix[b, HALO:, :] = m.astype(F32)
        tail[l, b] = m[T - HALO:, :]

    def project_outer(l, b):
        n = normed[block(b), :]
        outer[block(b), :] = jnp.dot(n, win[l, 2], preferred_element_type=F32)

    def send_tail(l, b, n):
        near = jnp.logical_or(x == 0, b == 0)
        far = jnp.logical_and(tail_out, b == 1)
        src, to = tail.at[l, b], jnp.minimum(b + x, 1)
        send(TAIL + n, src, halo.at[l, to], halo_recv.at[l, to], x_dev, l, near)
        send(TAIL + n, src, halo.at[l, 0], halo_recv.at[l, 0], (sp + 3, tp), l, far)

    def convolve(l, b):
        first = jnp.logical_and(jnp.logical_and(x == 0, b == 0), jnp.logical_not(has_down))
        mix[b, 0:HALO, :] = jnp.zeros((HALO, nb), F32)

        @pl.when(jnp.logical_not(first))
        def _():
            await_recv(halo.at[l, b], halo_recv.at[l, b])
            mix[b, 0:HALO, :] = halo[l, b].astype(F32)

        tap = taps[:, l, col(q)]
        o = HALO - 8

        def body(i, carry):
            m = mix[b, pl.ds(pl.multiple_of(o + i * mb, 8), mb + 8), :]
            conv = tap[0:1] * m[6:6 + mb] + tap[1:2] * m[7:7 + mb] + tap[2:3] * m[8:8 + mb]
            rows = pl.ds(pl.multiple_of(b * T + i * mb, mb), mb)
            gated[rows, :] = (outer[rows, :] * conv).astype(BF16)
            return carry
        lax.fori_loop(0, mper, body, 0)

    per_tp = SP // TP

    def w_block(l, j):
        return jnp.concatenate([wout[l, j * per_tp + p] for p in range(per_tp)], axis=1)

    def product(l, b, yj, core):
        return jnp.dot(gated[block(b), :], w_block(l, 2 * yj + core),
                       preferred_element_type=F32).astype(BF16)

    def f(ref):
        return ref.astype(F32)

    order = ((1 - q, 1 - y), (q, 1 - y), (1 - q, y), (q, y))

    def y_first(l, h):
        return l + 1 < L or h == 0

    def outputs(l):
        for b, yj in order:
            tsend[l, b, yj] = product(l, b, yj, 1 - c)
            send(PARTIAL, tsend.at[l, b, yj], r1.at[l, b, yj], r1_recv.at[l, b, yj], c_dev, l)
        for k, (b, yj) in enumerate(order):
            t = product(l, b, yj, c)
            await_recv(r1.at[l, b, yj], r1_recv.at[l, b, yj])
            s1[l, b, yj] = (f(t) + f(r1[l, b, yj])).astype(BF16)
            for h in range(2):
                rows = rows_of[h]
                if y_first(l, h) and k in (0, 1):
                    at, dev = b, y_dev
                elif not y_first(l, h) and k in (0, 2):
                    at, dev = yj, pair_dev
                else:
                    continue
                send(FIRST, s1.at[l, b, yj, rows, :], ra.at[l, at, rows, :],
                     ra_recv.at[l, at, h], dev, l)

    def reduce_second(l, h):
        rows = rows_of[h]
        if y_first(l, h):
            at, mine, dev = 1 - q, (1 - q, y), pair_dev
        else:
            at, mine, dev = 1 - y, (q, 1 - y), y_dev
        await_recv(ra.at[l, at, rows, :], ra_recv.at[l, at, h])
        s2[l, rows, :] = (f(s1[l, mine[0], mine[1], rows, :]) + f(ra[l, at, rows, :])).astype(BF16)
        send(SECOND, s2.at[l, rows, :], rb.at[l, rows, :], rb_recv.at[l, h], dev, l)

    def reduce_last(l, h):
        rows = rows_of[h]
        at = q if y_first(l, h) else y
        await_recv(ra.at[l, at, rows, :], ra_recv.at[l, at, h])
        await_recv(rb.at[l, rows, :], rb_recv.at[l, h])
        branch = f(s1[l, q, y, rows, :]) + f(ra[l, at, rows, :]) + f(rb[l, rows, :])
        return (f(held[l, q, tp, rows, :]) + branch).astype(BF16)

    for l in range(L):
        for i in range(4):
            local_copy(l, i).start()
    held[0, q, tp] = stream[...]

    barrier = pltpu.get_barrier_semaphore()
    count = 4
    for dev in (x_dev, y_dev, c_dev, pair_dev):
        pl.semaphore_signal(barrier, inc=1, device_id=dev, device_id_type=MESH)
    others = [(inside(z - ahead), (sp - 2 * ahead, tp))]
    for d in range(2, reach(0, 0) + 1):
        for way in (-1, 1):
            others.append((inside(z + way * d), (sp + 2 * way * d, tp)))
    for cond, dev in others:
        count = count + cond.astype(jnp.int32)

        @pl.when(cond)
        def _(dev=dev):
            pl.semaphore_signal(barrier, inc=1, device_id=dev, device_id_type=MESH)

    @pl.when(tail_in)
    def _():
        pl.semaphore_signal(barrier, inc=1, device_id=(sp - 3, tp), device_id_type=MESH)
    pl.semaphore_wait(barrier, count + tail_out.astype(jnp.int32))

    def gather_first(l):
        for h in range(2):
            gather_pair(l, h)
            gather_y(l, q, h)

    def gather_last(l):
        for h in range(2):
            gather_y(l, 1 - q, h)

    def project(l, b):
        project_mix(l, b)
        send_tail(l, b, 0 if b is q else 1)

    def finish(l):
        turn = jnp.where(x == 1, q, 1 - q)
        convolve(l, turn)
        convolve(l, 1 - turn)
        weights_ready(l, 3)
        outputs(l)

    def flush_weights(l):
        size = lambda n: win.at[l, 0, pl.ds(0, n * kp), :]
        for side in range(2):
            for d in range(1, Z):
                to = z + ways[side] * d
                n = sum(d <= reach(l, k) for k in range(KINDS))
                if n:
                    await_send(size(n), own_sems.at[l, 3 * (1 - side) + d - 1], inside(to))
                n = sum(relayed_of(l, k, d, Z) for k in range(KINDS))
                if n:
                    both = jnp.logical_and(inside(to), inside(z - 2 * ways[side]))
                    await_send(size(n), relay_sems.at[relays.index((l, d)), side], both)
        for o in range(Z):
            await_send(size(KINDS), fwd_sems.at[l, o])

    def flush_gather(l):
        await_send(held.at[l, 0], send_sems.at[l, RELAY])
        await_send(ra.at[l], send_sems.at[l, OWN])
        await_send(rb.at[l], send_sems.at[l, OWN_CORE])

    def flush_layer(l):
        await_send(tsend.at[l], send_sems.at[l, PARTIAL])
        await_send(ra.at[l], send_sems.at[l, FIRST])
        await_send(rb.at[l], send_sems.at[l, SECOND])
        for n, b in ((0, q), (1, 1 - q)):
            near = jnp.logical_or(x == 0, b == 0)
            far = jnp.logical_and(tail_out, b == 1)
            await_send(tail.at[l, 0], send_sems.at[l, TAIL + n], jnp.logical_or(near, far))

    def advance(l, store):
        n = l + 1
        if n == L:
            for h in range(2):
                reduce_second(l, h)
            for m in range(L):
                flush_weights(m)
                flush_gather(m)
                if m < l:
                    flush_layer(m)
            for h in range(2):
                store(h, reduce_last(l, h))
            return
        if n > 1:
            issue(n, 2)
        take_near(n, *pieces(0))
        reduce_second(l, 0)
        take_near(n, *pieces(1))
        reduce_second(l, 1)
        store(0, reduce_last(l, 0))
        take_far(n, *pieces(0))
        store(1, reduce_last(l, 1))
        take_far(n, *pieces(1))
        take_near(n, *pieces(2))
        take_far(n, *pieces(2))

    inner = inside(z - ahead)
    outer_end = jnp.logical_not(inner)
    for h in range(2):
        spread_own(0, h)
    for k in range(KINDS):
        own_x(0, k)
        toward(0, k)
        away(0, k)
        if k == SPLIT - 1:
            spread(OWN, 0, q, 0, FROM_PAIR)
            spread(OWN, 0, q, 1, FROM_PAIR, inner)
        if k == 2 * SPLIT - 1:
            spread(OWN, 0, q, 1, FROM_PAIR, outer_end)

    def first_arrivals():
        for k in range(SPLIT):
            take_near(0, k)
        for h in range(2):
            gather_y(0, q, h)
        for k in range(SPLIT, 2 * SPLIT):
            take_others(0, k)
            take_pair(0, k, inner)
            if k == SPLIT:
                gather_pair(0, 0)
                gather_core(0, q)
                normalize(0, q)
        for k in pieces(2)[:1]:
            take_others(0, k, inner)
            take_pair(0, k, inner)
        gather_pair(0, 1)
        for k in pieces(2)[:1]:
            take_others(0, k, outer_end)
        for k in pieces(1) + pieces(2)[:1]:
            take_pair(0, k, outer_end)
        take_near(0, *pieces(2)[1:])
        gather_last(0)
        take_near(0, *pieces(3)[:-1])
        gather_core(0, 1 - q)
        normalize(0, 1 - q)
        weights_ready(0, 0)
        weights_ready(0, 1)
        project(0, q)
        take_near(0, *pieces(3)[-1:])
        take_far(0, *range(KINDS))
        project(0, 1 - q)

    for l in range(L):
        more = l + 1 < L
        if l == 0:
            first_arrivals()
            if more:
                issue(1, 0, 1, 2)
                for k in range(KINDS):
                    own_x(1, k)
            weights_ready(0, 2)
            project_outer(0, q)
            project_outer(0, 1 - q)
        else:
            for h in range(2):
                gather_y(l, q, h)
                gather_pair(l, h)
                if h == 0:
                    issue(l, 3)
            gather_core(l, q)
            normalize(l, q)
            if more:
                issue(l + 1, 0, 1)
                for k in range(KINDS):
                    own_x(l + 1, k)
            for i in range(3):
                weights_ready(l, i)
            project(l, q)
            project_outer(l, q)
            take_near(l, *pieces(3))
            take_far(l, *pieces(3))
            gather_last(l)
            gather_core(l, 1 - q)
            normalize(l, 1 - q)
            project(l, 1 - q)
            project_outer(l, 1 - q)
        finish(l)
        if more:
            def store(h, value, l=l):
                held[l + 1, q, tp, rows_of[h], :] = value
                spread(OWN, l + 1, q, h, FROM_PAIR)
                spread_own(l + 1, h)
            advance(l, store)
        else:
            def store(h, value):
                out[rows_of[h], :] = value
            advance(l, store)

    flush_layer(L - 1)


def on_device(SP, TP, stream, norm_gain, w_value, w_inner, w_outer, conv_taps, w_output):
    L, kb, cb = w_value.shape
    T, D = stream.shape[0], norm_gain.shape[1]
    nb, Z = cb // 2, SP // 2
    dims = (L, SP, TP, D, T, kb, nb, cb)
    vmem = pl.BlockSpec(memory_space=pltpu.VMEM)
    hbm = pl.BlockSpec(memory_space=pl.ANY)
    dma = pltpu.SemaphoreType.DMA
    kinds = 4 * SPLIT
    n_relays = max(1, len(relay_slots(L, Z)))
    return pl.pallas_call(
        functools.partial(kernel, dims),
        out_shape=jax.ShapeDtypeStruct((T, cb), BF16),
        in_specs=[vmem, vmem, hbm, hbm, hbm, vmem, hbm],
        out_specs=vmem,
        scratch_shapes=[
            pltpu.VMEM((L, 3, D, nb), BF16),
            pltpu.VMEM((L, SP, nb, kb), BF16),
            pltpu.VMEM((L, 2, TP, T, cb), BF16),
            pltpu.VMEM((2 * T, D), BF16),
            pltpu.VMEM((2, T + HALO, nb), F32),
            pltpu.VMEM((2 * T, nb), F32),
            pltpu.VMEM((2 * T, nb), BF16),
            pltpu.VMEM((L, 2, 2, T, cb), BF16),
            pltpu.VMEM((L, 2, 2, T, cb), BF16),
            pltpu.VMEM((L, 2, 2, T, cb), BF16),
            pltpu.VMEM((L, 2, T, cb), BF16),
            pltpu.VMEM((L, T, cb), BF16),
            pltpu.VMEM((L, T, cb), BF16),
            pltpu.VMEM((L, 2, HALO, nb), BF16),
            pltpu.VMEM((L, 2, HALO, nb), BF16),
            dma((L, 8)),
            dma((L, 6)),
            dma((L, Z)),
            dma((n_relays, 2)),
            dma((L, Z, kinds)),
            dma((L, 4)),
            dma((L, 4)),
            dma((L, 2, 2, 2)),
            dma((L, 2)),
            dma((L, 2, 2)),
            dma((L, 2, 2)),
            dma((L, 2)),
            dma((L, 2)),
        ],
        compiler_params=pltpu.CompilerParams(
            collective_id=0, has_side_effects=True, vmem_limit_bytes=60 * 1024 * 1024
        ),
    )(stream, norm_gain, w_value, w_inner, w_outer, jnp.transpose(conv_taps, (1, 0, 2)), w_output)


def solution(mesh):
    SP, TP = mesh.shape["sp"], mesh.shape["tp"]
    in_specs = (
        P("sp", "tp"),
        P(),
        P(None, "sp", "tp"),
        P(None, "sp", "tp"),
        P(None, "sp", "tp"),
        P(None, None, "tp"),
        P(None, "tp", "sp"),
    )
    return jax.shard_map(
        functools.partial(on_device, SP, TP),
        mesh=mesh, in_specs=in_specs, out_specs=P("sp", "tp"), check_vma=False,
    )
```
